32 devices in a mesh: ep: 8 (over z, y), tp: 4 (over x, core).
Axes of the slice: x: 2, y: 2, z: 4, core: 2. Of those that a mesh axis runs over, the one named last changes fastest.
Arguments:
- queries: bfloat16 [4096, 2048], P('ep', 'tp'), may hold values from -6 to 6
- key_rows: bfloat16 [4096, 2048], P('ep', 'tp'), may hold values from -6 to 6
- value_rows: bfloat16 [4096, 4096], P('ep', 'tp'), may hold values from -6 to 6
- gate_rows: bfloat16 [4096, 4096], P('ep', 'tp'), may hold values from -6 to 6
- log_decay: float32 [16, 4096], P('tp', 'ep'), may hold values from -1 to 0
- head_gain: float32 [4096], P('tp'), may hold values from 0.1 to 1.9
- out_weight: bfloat16 [4096, 4096], P('tp'), may hold values from -0.09375 to 0.09375
- expert_input: bfloat16 [4096, 4096], P('ep'), may hold values from -6 to 6
- input_gain: float32 [4096], replicated, may hold values from 0.1 to 1.9
- route_ids: int32 [4096, 2], P('ep'), may hold values from 0 to 7, as said below
- route_weight: float32 [4096, 2], P('ep'), may hold values from 0.1 to 0.9
- expert_gate: bfloat16 [8, 4096, 1024], P('ep', None, 'tp'), may hold values from -0.09375 to 0.09375
- expert_up: bfloat16 [8, 4096, 1024], P('ep', None, 'tp'), may hold values from -0.09375 to 0.09375
- expert_down: bfloat16 [8, 1024, 4096], P('ep', 'tp'), may hold values from -0.1875 to 0.1875
Outputs:
- mixer_out: bfloat16 [4096, 4096], P(('ep', 'tp'))
- expert_out: bfloat16 [4096, 4096], P('ep', 'tp')
The draws below stay inside these ranges and needn't reach their ends.
Inputs may be any that keep to these rules, and one draw needn't show every extreme that they name: `route_ids`: each row names two different experts of one group of 8 consecutive experts. On the rows of one device each group is named by exactly 512 rows, experts 2 i and 2 i + 1 together are named exactly 4 * 192 / 3 times, and no expert is named by more than 192 rows; one expert is named by exactly 192 rows of every device.
All inputs are finite; a program needn't handle non-finite values.
Results may differ from the reference program's by a relative error of at most 0.019.
Values may be sent and summed in bfloat16 or wider, within the bound.
No kernel may reach another device: no remote copies, remote signals or barrier semaphores. Data moves between devices by JAX's collectives and lax.ppermute only.
A program may use at most 192 MiB of HBM per device.

```python
import math
import jax
import jax.numpy as jnp
from jax import lax

D = 4096
HEADS = 16
DK = 128
DV = 256
FF = 1024
EPG = 8
BLOCK = 512
TOK_A = 512
TOK_B = 512
EXPERTS = 8
GROUPS = 1
CAP = 192
FIRST_TOKENS = 4096
TOKENS_B = 4096
N_EP = 8
N_TP = 4


def draw_log_decay(key, part):
    random_subkeys = jax.random.split(jax.random.fold_in(key, 11), 7)
    quick = jax.random.uniform(random_subkeys[0], (HEADS,), jnp.float32) < 0.5
    quick_rate = 1.0 / jax.random.uniform(random_subkeys[1], (HEADS,), jnp.float32, 30.0, 50.0)
    steady_rate = 0.2 / FIRST_TOKENS * jnp.exp(jax.random.uniform(random_subkeys[2], (HEADS,), jnp.float32, -0.7, 0.0))
    head_rate = jnp.where(quick, quick_rate, steady_rate)
    shards = FIRST_TOKENS // TOK_A
    shard_factor = jnp.exp(jax.random.uniform(random_subkeys[3], (shards,), jnp.float32, 0.0, math.log(3.0)))
    position_factor = jnp.repeat(shard_factor, TOK_A, total_repeat_length=FIRST_TOKENS)
    roughness = jnp.exp(jax.random.uniform(random_subkeys[4], (HEADS, FIRST_TOKENS), jnp.float32, -0.35, 0.35))
    reference_level = -head_rate[:, None] * position_factor[None, :] * roughness
    spike_locations = jax.random.randint(random_subkeys[5], (2,), 0, FIRST_TOKENS)
    spike_removal = jnp.log(jax.random.uniform(random_subkeys[6], (2,), jnp.float32, 0.5, 0.8))
    spike_struck = (jnp.arange(FIRST_TOKENS)[None, :] == spike_locations[:, None]).astype(jnp.float32)
    spike_events = jnp.sum(spike_struck * spike_removal[:, None], axis=0)
    return reference_level + spike_events[None, :]


def route_block(block_key, busiest):
    random_subkeys = jax.random.split(block_key, 4)
    pair_count = EXPERTS // 2
    third = CAP // 3
    lifted = jax.random.randint(random_subkeys[0], (pair_count,), 0, 2 * third + 1)
    pair_index = jnp.arange(pair_count)
    lifted = jnp.where(pair_index == busiest // 2, 0, lifted)
    upper_side = jax.random.randint(random_subkeys[1], (pair_count,), 0, 2)
    upper_side = jnp.where(pair_index == busiest // 2, busiest % 2, upper_side)
    heavy = CAP - lifted
    lighter = third + lifted
    even_load = jnp.where(upper_side == 0, heavy, lighter)
    odd_load = jnp.where(upper_side == 0, lighter, heavy)
    loads = jnp.stack([even_load, odd_load], axis=1).reshape(GROUPS, EPG)
    run_ends = jnp.cumsum(loads, axis=1)
    group_rows = TOK_B // GROUPS
    tickets = jnp.arange(2 * group_rows)
    local_expert = jnp.sum((tickets[None, :, None] >= run_ends[:, None, :]).astype(jnp.int32), axis=2)
    shuffled = jax.random.permutation(random_subkeys[2], TOK_B)
    group_of = shuffled // group_rows
    place_of = shuffled % group_rows
    first_pick = group_of * EPG + local_expert[group_of, place_of]
    second_pick = group_of * EPG + local_expert[group_of, place_of + group_rows]
    swapped = jax.random.randint(random_subkeys[3], (TOK_B,), 0, 2)
    column_one = jnp.where(swapped == 0, first_pick, second_pick)
    column_two = jnp.where(swapped == 0, second_pick, first_pick)
    return jnp.stack([column_one, column_two], axis=1).astype(jnp.int32)


def draw_route_ids(key, part):
    busiest = jax.random.randint(jax.random.fold_in(key, 7), (), 0, EXPERTS)
    shards = TOKENS_B // TOK_B
    stacked = jax.vmap(lambda shard_index: route_block(jax.random.fold_in(key, shard_index + 100), busiest))(jnp.arange(shards))
    return stacked.reshape(TOKENS_B, 2)


def level_of(rng, extent, cuts, smallest, largest):
    loudness, own = 1.0, jax.random.fold_in(rng, 6)
    for position, parts in cuts:
        steps = jnp.exp(jax.random.uniform(jax.random.fold_in(own, position), (parts,), jnp.float32, smallest / len(cuts), largest / len(cuts)))
        loudness = loudness * jnp.repeat(steps, extent[position] // parts).reshape([-1 if axis == position else 1 for axis in range(len(extent))])
    return loudness


def normal_values(rng, extent, scale, limit, cuts=(), kind=jnp.bfloat16):
    level = level_of(rng, extent, cuts, -0.22, 0.18) if cuts else 1.0
    entries = jax.random.normal(rng, extent, jnp.float32) * scale * level
    return jnp.minimum(jnp.maximum(entries, -limit), limit).astype(kind)


def setup_inputs(seed: int = 0) -> dict:
    keys = jax.random.split(jax.random.key(seed), 15)
    queries = normal_values(keys[0], (FIRST_TOKENS, HEADS * DK), 1.0, 6.0, ((0, 8), (1, 4)))
    key_rows = normal_values(keys[1], (FIRST_TOKENS, HEADS * DK), 1.0, 6.0, ((0, 8), (1, 4)))
    value_rows = normal_values(keys[2], (FIRST_TOKENS, HEADS * DV), 1.0, 6.0, ((0, 8), (1, 4)))
    gate_rows = normal_values(keys[3], (FIRST_TOKENS, HEADS * DV), 1.0, 6.0, ((0, 8), (1, 4)))
    log_decay = draw_log_decay(jax.random.fold_in(keys[14], 71), 0)
    head_gain = jnp.clip(1.0 + 0.18 * jax.random.normal(keys[5], (HEADS * DV,), jnp.float32), 0.1, 1.9)
    out_weight = normal_values(keys[6], (HEADS * DV, D), (HEADS * DV) ** -0.5, 0.09375, ((0, 4),))
    expert_input = normal_values(keys[7], (TOKENS_B, D), 1.0, 6.0, ((0, 8),))
    input_gain = jnp.clip(1.0 + 0.18 * jax.random.normal(keys[8], (D,), jnp.float32), 0.1, 1.9)
    route_ids = draw_route_ids(jax.random.fold_in(keys[14], 71), 0)
    route_weight = jnp.clip(0.1 + 0.79999997 * jax.random.uniform(keys[10], (TOKENS_B, 2), jnp.float32) ** level_of(keys[10], (TOKENS_B, 2), ((0, 8),), -0.2, 0.2), 0.1, 0.9)
    expert_gate = normal_values(keys[11], (EXPERTS, D, FF), D ** -0.5, 0.09375, ((0, 8), (2, 4)))
    expert_up = normal_values(keys[12], (EXPERTS, D, FF), D ** -0.5, 0.09375, ((0, 8), (2, 4)))
    expert_down = normal_values(keys[13], (EXPERTS, FF, D), FF ** -0.5, 0.1875, ((0, 8), (1, 4)))
    return dict(queries=queries, key_rows=key_rows, value_rows=value_rows, gate_rows=gate_rows, log_decay=log_decay, head_gain=head_gain, out_weight=out_weight, expert_input=expert_input, input_gain=input_gain, route_ids=route_ids, route_weight=route_weight, expert_gate=expert_gate, expert_up=expert_up, expert_down=expert_down)


epsilon = 1e-06
theta_base = 10000.0
largest_entry = lax.Precision.HIGHEST

def rotate(values, positions):
    half_dim = values.shape[-1] // 2
    frequency = theta_base ** (-jnp.arange(half_dim, dtype=jnp.float32) / half_dim)
    angles = positions.astype(jnp.float32)[:, None, None] * frequency
    cosine = jnp.cos(angles)
    sine_wave = jnp.sin(angles)
    first_half = values[..., :half_dim]
    second = values[..., half_dim:]
    return jnp.concatenate([first_half * cosine - second * sine_wave, second * cosine + first_half * sine_wave], axis=-1)

def round_back(values):
    return lax.optimization_barrier(values.astype(jnp.bfloat16)).astype(jnp.float32)

def grouped_product(hidden, weight, groups):
    width = hidden.shape[1] // groups
    summed = jnp.zeros((hidden.shape[0], weight.shape[1]), jnp.float32)
    for group_index in range(groups):
        lower = group_index * width
        partial_sum = jnp.dot(hidden[:, lower:lower + width], weight[lower:lower + width], preferred_element_type=jnp.float32)
        summed = summed + round_back(partial_sum)
    return summed.astype(jnp.bfloat16)

def to_blocks(array, blocks):
    return array.reshape(blocks, array.shape[0] // blocks, array.shape[1], array.shape[2])

def retention(queries, key_rows, value_rows, gate_rows, log_decay, head_gain):
    tokens_all = queries.shape[0]
    positions = jnp.arange(tokens_all, dtype=jnp.int32)
    blocks = tokens_all // BLOCK
    query_rot = to_blocks(rotate(queries.astype(jnp.float32).reshape(tokens_all, HEADS, DK), positions), blocks)
    key_rot = to_blocks(rotate(key_rows.astype(jnp.float32).reshape(tokens_all, HEADS, DK), positions) * DK ** (-0.5), blocks)
    value_all = to_blocks(value_rows.astype(jnp.float32).reshape(tokens_all, HEADS, DV), blocks)
    running = jnp.cumsum(log_decay.reshape(HEADS, blocks, BLOCK), axis=2)
    causal = jnp.arange(BLOCK)[:, None] >= jnp.arange(BLOCK)[None, :]

    def advance(carried, inputs):
        query_tile, key_tile, value_blk, running_blk = inputs
        spread = running_blk[:, :, None] - running_blk[:, None, :]
        weight_table = jnp.exp(jnp.where(causal[None], spread, -jnp.inf))
        score_matrix = jnp.einsum('xya,zya->yxz', query_tile, key_tile, precision=largest_entry) * weight_table
        inside = jnp.einsum('hlm,mhe->lhe', score_matrix, value_blk, precision=largest_entry)
        outside = jnp.einsum('lhd,hl,hde->lhe', query_tile, jnp.exp(running_blk), carried, precision=largest_entry)
        ending = running_blk[:, -1]
        kept = jnp.exp(ending[:, None] - running_blk)
        updated = jnp.exp(ending)[:, None, None] * carried + jnp.einsum('lhd,hl,lhe->hde', key_tile, kept, value_blk, precision=largest_entry)
        return (updated, inside + outside)
    final_state, mixed = lax.scan(advance, jnp.zeros((HEADS, DK, DV), jnp.float32), (query_rot, key_rot, value_all, jnp.moveaxis(running, 1, 0)))
    mixed = mixed.reshape(tokens_all, HEADS, DV)
    centered = mixed - lax.optimization_barrier(jnp.mean(mixed, axis=-1, keepdims=True))
    normed = centered * lax.rsqrt(lax.optimization_barrier(jnp.mean(centered * centered, axis=-1, keepdims=True)) + epsilon) * head_gain.reshape(HEADS, DV)
    return (jax.nn.silu(gate_rows.astype(jnp.float32)) * normed.reshape(tokens_all, HEADS * DV)).astype(jnp.bfloat16)

def expert_layer(expert_input, input_gain, route_ids, route_weight, expert_gate, expert_up, expert_down):
    tokens_all = expert_input.shape[0]
    widened = expert_input.astype(jnp.float32)
    normed = (widened * lax.rsqrt(lax.optimization_barrier(jnp.mean(widened * widened, axis=-1, keepdims=True)) + epsilon) * input_gain).astype(jnp.bfloat16)
    padded = jnp.concatenate([normed, jnp.zeros((1, D), jnp.bfloat16)], axis=0)
    slots = N_EP * CAP
    flat_ids = route_ids.reshape(-1).astype(jnp.int32)
    matches = (flat_ids[:, None] == jnp.arange(EXPERTS, dtype=jnp.int32)[None, :]).astype(jnp.int32)
    slot_rank = lax.optimization_barrier(jnp.sum((jnp.cumsum(matches, axis=0) - matches) * matches, axis=1)).astype(jnp.int32)
    target = (flat_ids * slots + slot_rank).astype(jnp.int32)
    owners = (jnp.arange(2 * tokens_all, dtype=jnp.int32) // 2).astype(jnp.int32)
    slot_table = jnp.full((EXPERTS * slots,), tokens_all, jnp.int32).at[target].set(owners)

    def one_expert(inputs):
        row_index, gate_matrix, up_matrix, down_matrix = inputs
        chosen = padded[row_index]
        gate_val = jnp.dot(chosen, gate_matrix, preferred_element_type=jnp.float32)
        up_val = jnp.dot(chosen, up_matrix, preferred_element_type=jnp.float32)
        inner_rows = (jax.nn.silu(gate_val) * up_val).astype(jnp.bfloat16)
        return grouped_product(inner_rows, down_matrix, N_TP)
    results = lax.map(one_expert, (slot_table.reshape(EXPERTS, slots), expert_gate, expert_up, expert_down))
    picked = results.reshape(EXPERTS * slots, D)[target].reshape(tokens_all, 2, D).astype(jnp.float32)
    return lax.optimization_barrier(jnp.sum(picked * route_weight[:, :, None], axis=1)).astype(jnp.bfloat16)

def reference(queries, key_rows, value_rows, gate_rows, log_decay, head_gain, out_weight, expert_input, input_gain, route_ids, route_weight, expert_gate, expert_up, expert_down):
    hidden = retention(queries, key_rows, value_rows, gate_rows, log_decay, head_gain)
    mixer_out = grouped_product(hidden, out_weight, N_TP)
    expert_out = expert_layer(expert_input, input_gain, route_ids, route_weight, expert_gate, expert_up, expert_down)
    return (mixer_out, expert_out)
```

```python
import functools

import jax
import jax.numpy as jnp
from jax import lax
from jax.experimental import pallas as pl
from jax.experimental.pallas import tpu as pltpu
from jax.sharding import PartitionSpec as P


epsilon = 1e-06
theta_base = 10000.0
f32, bf16 = jnp.float32, jnp.bfloat16


def swap(value, axis, mask):
    size = lax.axis_size(axis)
    return lax.ppermute(value, axis, [(i, i ^ mask) for i in range(size)])


def dot(a, b):
    return jnp.dot(a, b, preferred_element_type=f32)


def turn(v, cosine, sine):
    half = v.shape[-1] // 2
    other = jnp.concatenate([v[:, half:], v[:, :half]], axis=-1)
    return v * cosine + other * sine


def split(v):
    high = v.astype(bf16)
    return high, (v - high.astype(f32)).astype(bf16)


def contract(a, b, dims):
    return lax.dot_general(a, b, (dims, ((), ())), preferred_element_type=f32)


def message(state, decay):
    high = decay.astype(bf16).astype(f32)
    tail = jnp.concatenate([high, decay - high], axis=-2)
    return state.astype(bf16), tail.astype(bf16)


def inside_kernel(
    q_ref, k_ref, v_ref, cos_ref, sin_ref, log_ref, o_ref, qd_ref, s_ref, d_ref, m_ref, rows, cols
):
    length, width = q_ref.shape
    out = v_ref.shape[1]
    heads = log_ref.shape[0]
    head = pl.program_id(0)
    later = lax.broadcasted_iota(jnp.int32, (length, length), 0)
    earlier = lax.broadcasted_iota(jnp.int32, (length, length), 1)
    causal = later >= earlier

    @pl.when(head == 0)
    def _():
        log = log_ref[...]
        high = log.astype(bf16).astype(f32)
        middle = (log - high).astype(bf16).astype(f32)
        ones = jnp.where(causal, 1.0, 0.0).astype(bf16)
        pad = jnp.zeros((8 - heads, length), f32)
        row, col = 0.0, 0.0
        for piece in (high, middle, log - high - middle):
            piece = jnp.concatenate([piece, pad], axis=0).astype(bf16)
            row += contract(piece, ones, ((1,), (1,)))
            col += contract(ones, piece, ((1,), (1,)))
        rows[...] = row
        cols[...] = col

    cosine, sine = cos_ref[...], sin_ref[...]
    q = turn(q_ref[...].astype(f32), cosine, sine)
    k = turn(k_ref[...].astype(f32), cosine, sine) * width ** (-0.5)
    v = v_ref[...]
    row = rows[pl.ds(head, 1), :]
    which = lax.broadcasted_iota(jnp.int32, (length, 8), 1)
    col = jnp.sum(jnp.where(which == head, cols[...], 0.0), axis=1, keepdims=True)
    ending = row[:, length - 1 :]
    kept_high, kept_low = split(k * jnp.exp(ending - col))
    kept = contract(jnp.concatenate([kept_high, kept_low], axis=1), v, ((0,), (0,)))
    state = kept[:width] + kept[width:]
    decay = jnp.broadcast_to(jnp.exp(ending), (8, out))
    s_ref[0] = state
    d_ref[0] = decay
    m_ref[0, :width], m_ref[0, width:] = message(state, decay)
    q_high, q_low = split(q)
    k_high, k_low = split(k)
    q_both = jnp.concatenate([q_high, q_low], axis=1)
    k_twice = jnp.concatenate([k_high, k_high], axis=1)
    last = ((1,), (1,))
    scores = contract(q_both, k_twice, last) + contract(q_high, k_low, last)
    weight = jnp.exp(jnp.where(causal, col - row, -jnp.inf))
    o_ref[...] = dot((scores * weight).astype(bf16), v)
    qd_ref[...] = q * jnp.exp(col)


def combine_kernel(late_ref, got_ref, s_ref, d_ref, *refs):
    width = s_ref.shape[1]
    late = late_ref[0] > 0
    other = got_ref[:, :width].astype(f32)
    tail = got_ref[:, width:].astype(f32)
    other_decay = tail[:, :8] + tail[:, 8:]
    state, decay = s_ref[...], d_ref[...]
    if len(refs) in (3, 7):
        before, before_decay = refs[0][...], refs[1][...]
        outs = refs[2:]
        outs[0][...] = jnp.where(late, before_decay[:, :1] * other + before, before)
    else:
        before_decay = jnp.ones_like(decay)
        outs = refs
        outs[0][...] = jnp.where(late, other, 0.0)
    if len(outs) == 1:
        return
    outs[1][...] = jnp.where(late, before_decay * other_decay, before_decay)
    state = jnp.where(late, decay[:, :1] * other + state, other_decay[:, :1] * state + other)
    decay = decay * other_decay
    outs[2][...] = state
    outs[3][...] = decay
    outs[4][:, :width], outs[4][:, width:] = message(state, decay)


def outside_kernel(o_ref, qd_ref, s_ref, gate_ref, gain_ref, h_ref):
    q_high, q_low = split(qd_ref[...])
    state = s_ref[0].astype(bf16)
    o = o_ref[...] + (dot(q_high, state) + dot(q_low, state))
    centered = o - jnp.mean(o, axis=-1, keepdims=True)
    scale = lax.rsqrt(jnp.mean(centered * centered, axis=-1, keepdims=True) + epsilon)
    gate = gate_ref[...].astype(f32)
    h_ref[...] = (gate / (1.0 + jnp.exp(-gate)) * (centered * scale * gain_ref[...])).astype(bf16)


def shapes(*arrays):
    return [jax.ShapeDtypeStruct(a.shape, a.dtype) for a in arrays]


def combine(final, late, got, state, decay, *before):
    results = [state, decay, state, decay, got]
    results = results[:1] if final else results
    return pl.pallas_call(
        combine_kernel,
        in_specs=[pl.BlockSpec(memory_space=pltpu.SMEM)] + [pl.BlockSpec()] * (3 + len(before)),
        out_shape=shapes(*results),
        name="combine",
    )(late, got, state, decay, *before)


def retention_inside(queries, key_rows, value_rows, log_decay):
    length = queries.shape[0]
    heads = log_decay.shape[0]
    width = queries.shape[1] // heads
    out = value_rows.shape[1] // heads
    half = width // 2
    positions = lax.axis_index("ep") * length + jnp.arange(length, dtype=jnp.int32)
    frequency = theta_base ** (-jnp.arange(half, dtype=f32) / half)
    angles = positions.astype(f32)[:, None] * frequency
    cosine, sine = jnp.cos(angles), jnp.sin(angles)
    cosine = jnp.concatenate([cosine, cosine], axis=-1)
    sine = jnp.concatenate([-sine, sine], axis=-1)
    whole = lambda *shape: pl.BlockSpec(shape, lambda h: (0,) * len(shape))
    cols = lambda n: pl.BlockSpec((length, n), lambda h: (0, h))
    first = lambda *shape: pl.BlockSpec((1,) + shape, lambda h: (h, 0, 0))
    return pl.pallas_call(
        inside_kernel,
        grid=(heads,),
        in_specs=[
            cols(width),
            cols(width),
            cols(out),
            whole(length, width),
            whole(length, width),
            whole(heads, length),
        ],
        out_specs=[cols(out), cols(width), first(width, out), first(8, out), first(width + 16, out)],
        out_shape=[
            jax.ShapeDtypeStruct((length, heads * out), f32),
            jax.ShapeDtypeStruct((length, heads * width), f32),
            jax.ShapeDtypeStruct((heads, width, out), f32),
            jax.ShapeDtypeStruct((heads, 8, out), f32),
            jax.ShapeDtypeStruct((heads, width + 16, out), bf16),
        ],
        scratch_shapes=[pltpu.VMEM((8, length), f32), pltpu.VMEM((length, 8), f32)],
        cost_estimate=pl.CostEstimate(
            flops=8 * heads * length * length * out, bytes_accessed=2**23, transcendentals=2**21
        ),
        name="inside",
    )(queries, key_rows, value_rows, cosine, sine, log_decay)


def retention_outside(inside, turned, incoming, gate_rows, head_gain):
    length = inside.shape[0]
    heads, width, out = incoming.shape
    cols = lambda n: pl.BlockSpec((length, n), lambda h: (0, h))
    first = lambda *shape: pl.BlockSpec((1,) + shape, lambda h: (h, 0, 0))
    return pl.pallas_call(
        outside_kernel,
        grid=(heads,),
        in_specs=[
            cols(out),
            cols(width),
            first(width, out),
            cols(out),
            pl.BlockSpec((1, out), lambda h: (0, h)),
        ],
        out_specs=cols(out),
        out_shape=jax.ShapeDtypeStruct((length, heads * out), bf16),
        cost_estimate=pl.CostEstimate(
            flops=8 * length * heads * out * width, bytes_accessed=2**22, transcendentals=2**19
        ),
        name="outside",
    )(inside, turned, incoming, gate_rows, head_gain[None, :])


def mixer_kernel(core_ref, hidden_ref, weight_ref, sent_ref, kept_ref, rows_ref):
    rows = hidden_ref.shape[0] // 4

    @pl.when(pl.program_id(0) == 0)
    def _():
        for i in range(4):
            core = 1 - core_ref[0] if i < 2 else core_ref[0]
            start = (2 * (i % 2) + core) * rows
            rows_ref[i * rows : (i + 1) * rows] = hidden_ref[pl.ds(start, rows), :]

    part = dot(rows_ref[...], weight_ref[...]).astype(bf16)
    sent_ref[...] = part[: 2 * rows]
    kept_ref[...] = part[2 * rows :]


def mixer_parts(hidden, out_weight, core):
    rows, width = hidden.shape
    model = out_weight.shape[1]
    tile = model // 8
    shape = jax.ShapeDtypeStruct((rows // 2, model), bf16)
    spec = pl.BlockSpec((rows // 2, tile), lambda j: (0, j))
    return pl.pallas_call(
        mixer_kernel,
        grid=(model // tile,),
        in_specs=[
            pl.BlockSpec(memory_space=pltpu.SMEM),
            pl.BlockSpec((rows, width), lambda j: (0, 0)),
            pl.BlockSpec((width, tile), lambda j: (0, j)),
        ],
        out_specs=[spec, spec],
        out_shape=[shape, shape],
        scratch_shapes=[pltpu.VMEM((rows, width), bf16)],
        cost_estimate=pl.CostEstimate(
            flops=2 * rows * width * model, bytes_accessed=2 * width * model, transcendentals=0
        ),
        name="mixer",
    )(core, hidden, out_weight)


def pick_kernel(plan, slot_ref, rows_ref, gain_ref, *refs):
    outs, sums = refs[:-1], refs[-1]
    tokens, model = rows_ref.shape
    first, second = slot_ref[0:1, :], slot_ref[1:2, :]
    hits = []
    for blocks in plan:
        for start, size in blocks:
            wanted = start + lax.broadcasted_iota(jnp.int32, (size, tokens), 0)
            hits.append(jnp.where((first == wanted) | (second == wanted), 1.0, 0.0))
    hit = jnp.concatenate(hits, axis=0).astype(bf16)
    square = jnp.zeros((hit.shape[0], 1), f32)
    tile = model // 8
    for j in range(8):
        part = dot(hit, rows_ref[:, j * tile : (j + 1) * tile])
        square += jnp.sum(part * part, axis=1, keepdims=True)
        sums[:, j * tile : (j + 1) * tile] = part
    scale = lax.rsqrt(square / model + epsilon)
    start = 0
    for out_ref, blocks in zip(outs, plan):
        size = sum(n for _, n in blocks)
        out_ref[...] = (
            sums[start : start + size, :] * scale[start : start + size] * gain_ref[...]
        ).astype(bf16)
        start += size


def picked(plan, slot, rows, gain):
    tokens, model = rows.shape
    heights = [sum(n for _, n in blocks) for blocks in plan]
    return pl.pallas_call(
        functools.partial(pick_kernel, plan),
        out_shape=[jax.ShapeDtypeStruct((n, model), bf16) for n in heights],
        scratch_shapes=[pltpu.VMEM((sum(heights), model), f32)],
        cost_estimate=pl.CostEstimate(
            flops=2 * sum(heights) * tokens * model, bytes_accessed=2**23, transcendentals=0
        ),
        name="pick",
    )(slot, rows, gain[None, :])


def inner_kernel(count, *refs):
    parts, weights, out_ref, sums = refs[:count], refs[count:-2], refs[-2], refs[-1]
    step = pl.program_id(0)
    rows = jnp.concatenate([r[...].reshape(-1, r.shape[-1]) for r in parts], axis=0)
    units = weights[0].shape[1]

    @pl.when(step == 0)
    def _():
        sums[...] = jnp.zeros_like(sums)

    for i, w in enumerate(weights):
        sums[:, i * units : (i + 1) * units] += dot(rows, w[...])

    @pl.when(step == pl.num_programs(0) - 1)
    def _():
        gate_val, up_val = sums[:, : 2 * units], sums[:, 2 * units :]
        out_ref[...] = (gate_val / (1.0 + jnp.exp(-gate_val)) * up_val).astype(bf16)


def inner_of(parts, weights, size):
    model, units = weights[0].shape
    depth = model // 4
    height = size * len(parts)
    specs = []
    for array, start in parts:
        if array.ndim == 3:
            spec = pl.BlockSpec((1, size, depth), lambda d, start=start: (start, 0, d))
        else:
            block = start // size
            spec = pl.BlockSpec((size, depth), lambda d, block=block: (block, d))
        specs.append(spec)
    return pl.pallas_call(
        functools.partial(inner_kernel, len(parts)),
        grid=(model // depth,),
        in_specs=specs + [pl.BlockSpec((depth, units), lambda d: (d, 0))] * 4,
        out_specs=pl.BlockSpec((height, 2 * units), lambda d: (0, 0)),
        out_shape=jax.ShapeDtypeStruct((height, 2 * units), bf16),
        scratch_shapes=[pltpu.VMEM((height, 4 * units), f32)],
        cost_estimate=pl.CostEstimate(
            flops=8 * height * model * units,
            bytes_accessed=8 * model * units,
            transcendentals=height * units,
        ),
        name="inner",
    )(*[a for a, _ in parts], *weights)


class Order:
    def __init__(self):
        self.last = None

    def __call__(self, stage, *inputs):
        if self.last is not None:
            inputs, _ = lax.optimization_barrier((inputs, self.last))
        result = stage(*inputs)
        self.last = jax.tree.leaves(result)[0]
        return result


def everything(
    queries,
    key_rows,
    value_rows,
    gate_rows,
    log_decay,
    head_gain,
    out_weight,
    expert_input,
    input_gain,
    route_ids,
    route_weight,
    expert_gate,
    expert_up,
    expert_down,
):
    then = Order()
    tokens, model = expert_input.shape
    ep = lax.axis_size("ep")
    rank, index = lax.axis_index("ep"), lax.axis_index("tp")
    y, z, x, c = rank % 2, rank // 2, index // 2, index % 2
    pairs = ep // 2
    quota = 2 * tokens // pairs // 4
    window = 3 * quota // 4
    units = expert_gate.shape[2]
    half, quarter = model // 2, model // 4
    groups = {
        "a": list(range(pairs // 2)),
        "b": list(range(pairs // 2, 3 * pairs // 4)),
        "c": list(range(3 * pairs // 4, pairs)),
    }
    sides_of = {"a": 2, "b": 1, "c": 1}
    alone = pairs == 4 and window % 16 == 0
    sent_of = groups
    if alone:
        groups, sent_of = {"a": [1], "b": [2], "c": [0, 3]}, {"a": [1], "b": [2], "c": [3]}
    size_of = {g: len(groups[g]) * window for g in groups}

    ids = route_ids.T.reshape(-1)
    one_hot = (ids[:, None] == jnp.arange(ep, dtype=jnp.int32)[None, :]).astype(f32)
    below = jnp.tril(jnp.ones((2 * tokens, 2 * tokens), bf16), -1)
    rank_of = dot(below, one_hot.astype(bf16))
    counts = jnp.sum(one_hot, axis=0)
    base = jnp.where(jnp.arange(ep) % 2 == y, 0.0, counts.reshape(pairs, 2)[:, ::-1].reshape(-1))
    place = jnp.sum(one_hot * (rank_of + base[None, :]), axis=1).astype(jnp.int32)
    turned = (place & 3) ^ index
    slot = (((ids >> 1) ^ z) * 4 + (turned & 1) * 2 + (turned >> 1)) * quota + (place >> 2)
    slot = slot.reshape(2, tokens)
    near_counts = jnp.where(y == 0, counts.reshape(pairs, 2)[:, 0], counts.reshape(pairs, 2)[:, 1])

    def blocks(ks, sides, low, n):
        return [((k * 4 + side) * quota + low, n) for side in range(sides) for k in ks]

    keys = ["c", "b", "a"]
    plan = [blocks(sent_of[g], sides_of[g], 0, quota) for g in keys]
    if alone:
        keys += ["far0", "near0"]
        plan += [blocks([0], 2, quota - window, window), blocks([0], 2, 0, window)]
    rows = dict(zip(keys, then(lambda *v: picked(plan, *v), slot, expert_input, input_gain)))

    def send_z(g):
        ks = sent_of[g]
        if len(ks) == 1:
            return swap(rows[g], "ep", 2 * ks[0])
        parts = rows[g].reshape(sides_of[g], len(ks), quota, model)
        return jnp.stack(
            [parts[:, j] if k == 0 else swap(parts[:, j], "ep", 2 * k) for j, k in enumerate(ks)],
            axis=1,
        )

    landed = {g: send_z(g) for g in ("c", "b", "a")}
    far, near, near_x, far_x = {}, {}, {}, {}
    if alone:
        near["0"], far["0"] = rows["near0"], swap(rows["far0"], "ep", 1)

    gate_own, up_own = expert_gate[0], expert_up[0]
    gate_other, up_other = swap(gate_own, "tp", 1), swap(up_own, "tp", 1)
    weights = (gate_own, gate_other, up_own, up_other)

    cut = lambda a, start, n: lax.dynamic_slice_in_dim(a, start, n, a.ndim - 1)
    down_own = expert_down[0]
    down_x, down_c = then(
        lambda d: (cut(d, (1 - x) * half, half), cut(d, x * half + (1 - c) * quarter, quarter)),
        down_own,
    )
    down_x, down_c = swap(down_x, "tp", 2), swap(down_c, "tp", 1)

    inside, queries_turned, state, decay, sent = then(
        retention_inside, queries, key_rows, value_rows, log_decay
    )
    got = swap(sent, "ep", 1)
    links = (state, decay)
    combine_step = 1

    def run_combine():
        nonlocal links, got, combine_step
        late = jnp.where((rank & combine_step) > 0, 1, 0).astype(jnp.int32).reshape(1)
        final = 2 * combine_step >= ep
        out = then(lambda *v: combine(final, *v), late, got, *links)
        combine_step *= 2
        if final:
            return out[0]
        links = (out[2], out[3], out[0], out[1])
        got = swap(out[4], "ep", combine_step)

    def split_rows(g):
        def stage(v):
            v = v.reshape(sides_of[g], -1, quota, model)
            f = v[:, :, quota - window :].reshape(-1, model)
            if alone and sides_of[g] == 2:
                return f, v[:, 0]
            return f, v[:, :, :window].reshape(-1, model)

        f, near[g] = then(stage, landed[g])
        far[g] = swap(f, "ep", 1)
        if sides_of[g] == 1:
            near_x[g] = swap(near[g], "tp", 2)

    def send_far(g):
        (f,) = then(lambda f: (f,), far[g])
        far[g], far_x[g] = f, swap(f, "tp", 2)

    inner, got_x, both, got_c = {}, {}, {}, {}

    def run_inner(g):
        parts, size = [], window if alone else size_of[g]
        for part, part_x in ((near, near_x), (far, far_x)):
            for side in range(2):
                if 0 in groups[g] and alone:
                    parts.append((part["0"], side * size))
                if sides_of[g] == 1:
                    parts.append(((part, part_x)[side][g], 0))
                else:
                    parts.append((part[g], side if part[g].ndim == 3 else side * size))
        starts = [start for _, start in parts]
        inner[g] = then(
            lambda *v: inner_of(list(zip(v, starts)), v[len(starts) :], size),
            *[p for p, _ in parts],
            *weights,
        )
        got_x[g] = swap(inner[g], "tp", 2)

    def run_both(g):
        def stage(own, other):
            other = other.reshape(2, 2, size_of[g], 2 * units)
            other = jnp.stack([other[:, 1], other[:, 0]], axis=1).reshape(own.shape)
            flip = [own[:, units:], own[:, :units], other[:, units:], other[:, :units]]
            return jnp.concatenate(flip, axis=1), jnp.concatenate([own, other], axis=1)

        flipped, both[g] = then(stage, inner[g], got_x[g])
        got_c[g] = swap(flipped, "tp", 1)

    result, result_far, back = {}, {}, {}

    def run_down(g):
        def rows_of(a, b, part):
            kept = slice(part * 2 * size_of[g], (part + 1) * 2 * size_of[g])
            return jnp.concatenate([a[kept], b[kept]], axis=0)

        out = then(lambda a, b, d: dot(rows_of(a, b, 1), d).astype(bf16), both[g], got_c[g], down)
        result_far[g] = swap(out, "ep", 1)
        result[g] = then(
            lambda a, b, d: dot(rows_of(a, b, 0), d).astype(bf16), both[g], got_c[g], down
        )

    def run_merge(g):
        ks = groups[g]

        def stage(n, f, l):
            n = n.reshape(2, 2, len(ks), window, quarter)
            f = f.reshape(2, 2, len(ks), window, quarter)
            pad = [(0, 0)] * 5
            pad[3] = (0, quota - window)
            n = jnp.pad(n, pad)
            pad[3] = (quota - window, 0)
            f = jnp.pad(f, pad)
            spot = lax.broadcasted_iota(f32, (2, 2, len(ks), quota, 1), 3)
            merged = jnp.where(spot < l[:, :, :, None, None], n, f)
            return [merged[:, :, j].reshape(4 * quota, quarter) for j in range(len(ks))]

        parts = then(stage, result[g], result_far[g], jnp.stack([limits[:, :, k] for k in ks], axis=2))
        for part, k in zip(parts, ks):
            back[k] = part if k == 0 else swap(part, "ep", 2 * k)

    def run_total(ks, total):
        def stage(slots, weight, total, *parts):
            for part, k in zip(parts, ks):
                places = k * 4 * quota + jnp.arange(4 * quota, dtype=jnp.int32)[None, :]
                mix = jnp.where(slots[0][:, None] == places, weight[:, :1], 0.0)
                mix += jnp.where(slots[1][:, None] == places, weight[:, 1:], 0.0)
                total = dot(mix.astype(bf16), part) + (0.0 if total is None else total)
            return total

        return then(stage, slot, route_weight, total, *[back[k] for k in ks])

    def half_rows(side):
        def stage(a, b):
            pick = lambda v: lax.dynamic_slice_in_dim(v, side * (tokens // 4), tokens // 4, 0)
            return pick(a).astype(f32) + pick(b).astype(f32)

        return stage

    split_rows("c")
    while 4 * combine_step < ep:
        run_combine()
    known = [near_counts] + [swap(near_counts, "ep", 2 * k) for k in range(1, pairs)]
    (down_c2,) = then(lambda d: (cut(d, (1 - c) * quarter, quarter),), down_x)
    down_c2 = swap(down_c2, "tp", 1)
    send_far("c")

    def build_down(own, x_got, c_got, c_got2):
        parts = [cut(own, index * quarter, quarter), c_got, cut(x_got, c * quarter, quarter), c_got2]
        return jnp.concatenate(parts, axis=0)

    down = then(build_down, down_own, down_x, down_c, down_c2)
    split_rows("b")
    run_inner("c")
    send_far("b")
    split_rows("a")
    run_both("c")

    def limits_of(known):
        turn_of = ((jnp.arange(2)[None, :] * 2 + jnp.arange(2)[:, None]) ^ index).astype(f32)
        numbers = lax.dynamic_slice_in_dim(jnp.stack(known), z, 1, 1)[:, 0]
        return jnp.ceil((numbers[None, None, :] - turn_of[:, :, None]) / 4)

    limits = then(limits_of, known)
    run_down("c")
    run_combine()
    run_inner("b")
    run_merge("c")
    incoming = run_combine()
    hidden = then(retention_outside, inside, queries_turned, incoming, gate_rows, head_gain)
    run_both("b")
    run_inner("a")
    run_down("b")
    mix_sent, mix_kept = then(mixer_parts, hidden, out_weight, c.astype(jnp.int32).reshape(1))
    mix_got = swap(mix_sent, "tp", 1)
    run_both("a")
    run_merge("b")
    run_down("a")
    mix_far = swap(
        then(lambda a, b: half_rows(1 - x)(a, b).astype(bf16), mix_kept, mix_got), "tp", 2
    )
    run_merge("a")
    total = run_total(groups["c"], None)
    mixer_out = then(
        lambda a, b, f: (half_rows(x)(a, b) + f.astype(f32)).astype(bf16), mix_kept, mix_got, mix_far
    )
    total = run_total(groups["a"], total)
    total = run_total(groups["b"], total)
    return (mixer_out, total.astype(bf16))


def solution(mesh):
    assert mesh.shape["tp"] == 4 and mesh.shape["ep"] & (mesh.shape["ep"] - 1) == 0
    placed = (
        P("ep", "tp"),
        P("ep", "tp"),
        P("ep", "tp"),
        P("ep", "tp"),
        P("tp", "ep"),
        P("tp"),
        P("tp", None),
        P("ep", None),
        P(),
        P("ep", None),
        P("ep", None),
        P("ep", None, "tp"),
        P("ep", None, "tp"),
        P("ep", "tp", None),
    )
    return jax.shard_map(
        everything,
        mesh=mesh,
        in_specs=placed,
        out_specs=(P(("ep", "tp"), None), P("ep", "tp")),
        check_vma=False,
    )
```
